32 devices in a mesh: ra: 8 (over z, y), cb: 4 (over x, core).
Axes of the slice: x: 2, y: 2, z: 4, core: 2. Of those that a mesh axis runs over, the one named last changes fastest.
Arguments:
- tokens: bfloat16 [512, 4096], P(None, 'cb'), may hold values from -82 to 82
- gate_weight: float32 [2, 4096, 11264], P(None, 'cb', 'ra'), may hold values from -0.09375 to 0.09375
- up_weight: float32 [2, 4096, 11264], P(None, 'cb', 'ra'), may hold values from -0.09375 to 0.09375
- down_weight: float32 [2, 11264, 4096], P(None, 'ra', 'cb'), may hold values from -0.0546875 to 0.0546875
- gate_scale: float32 [2, 11264], P(None, 'ra'), may hold values from 0.5 to 2
- up_scale: float32 [2, 11264], P(None, 'ra'), may hold values from 0.5 to 2
- down_scale: float32 [2, 4096], P(None, 'cb'), may hold values from 0.5 to 2
- norm_gain: float32 [2, 4096], P(None, 'cb'), may hold values from 0.1 to 1.9
- conv_taps: float32 [2, 3, 11264], P(None, None, 'ra'), may hold values from -3 to 3
- conv_bias: float32 [2, 11264], P(None, 'ra'), may hold values from -3 to 3
Outputs:
- layer_out: bfloat16 [512, 4096], P(None, 'cb')
The draws below stay inside these ranges and needn't reach their ends.
All inputs are finite; a program needn't handle non-finite values.
Results may differ from the reference program's by a relative error of at most 0.012.
Values may be sent and summed in bfloat16 or wider, within the bound.
A program may use at most 128 MiB of HBM per device.

```python
import math
import jax
import jax.numpy as jnp
from jax import lax

D = 4096
FF = 11264
TOKENS = 512
LAYERS = 2
KERNEL = 3


def draw_tokens(key, part):
    k_base, k_row, k_col = jax.random.split(key, 3)
    trend = jnp.linspace(0.0, math.log(10.0), D)
    jitter = jax.random.uniform(k_col, (D,), jnp.float32, -0.3, 0.3)
    column = jnp.exp(trend + jitter)
    row_scale = jnp.exp(jax.random.uniform(k_row, (TOKENS, 1), jnp.float32, 0.0, math.log(10.0)))
    base = jnp.clip(jax.random.normal(k_base, (TOKENS, D), jnp.float32), -6.0, 6.0)
    values = base * row_scale * column * 0.1
    return values.astype(jnp.bfloat16)


def level_of(own_key, shape, cuts, least, high):
    level, own = 1.0, jax.random.fold_in(own_key, 6)
    for axis_at, parts in cuts:
        steps = jnp.exp(jax.random.uniform(jax.random.fold_in(own, axis_at), (parts,), jnp.float32, least / len(cuts), high / len(cuts)))
        level = level * jnp.repeat(steps, shape[axis_at] // parts).reshape([-1 if axis == axis_at else 1 for axis in range(len(shape))])
    return level


def normal_values(stream_key, shape, width, bound, cuts=(), dtype=jnp.bfloat16):
    array = jax.random.normal(stream_key, shape, jnp.float32) * width
    if len(cuts) > 0:
        array = level_of(stream_key, shape, cuts, -0.22, 0.18) * array
    return jnp.clip(array, min=-bound, max=bound).astype(dtype)


def setup_inputs(seed: int = 0) -> dict:
    streams_of = jax.random.split(jax.random.key(seed), 11)
    return {
        "tokens": draw_tokens(jax.random.fold_in(streams_of[10], 71), 0),
        "gate_weight": normal_values(streams_of[1], (LAYERS, D, FF), D ** -0.5, 0.09375, ((1, 4), (2, 8)), jnp.float32),
        "up_weight": normal_values(streams_of[2], (LAYERS, D, FF), D ** -0.5, 0.09375, ((1, 4), (2, 8)), jnp.float32),
        "down_weight": normal_values(streams_of[3], (LAYERS, FF, D), FF ** -0.5, 0.0546875, ((1, 8), (2, 4)), jnp.float32),
        "gate_scale": jnp.clip(jnp.exp(math.log(2.0) - 1.3862944 * jax.random.uniform(streams_of[4], (LAYERS, FF), jnp.float32) ** level_of(streams_of[4], (LAYERS, FF), ((1, 8),), -0.2, 0.2)), 0.5, 2.0),
        "up_scale": jnp.clip(jnp.exp(math.log(2.0) - 1.3862944 * jax.random.uniform(streams_of[5], (LAYERS, FF), jnp.float32) ** level_of(streams_of[5], (LAYERS, FF), ((1, 8),), -0.2, 0.2)), 0.5, 2.0),
        "down_scale": jnp.clip(jnp.exp(math.log(2.0) - 1.3862944 * jax.random.uniform(streams_of[6], (LAYERS, D), jnp.float32) ** level_of(streams_of[6], (LAYERS, D), ((1, 4),), -0.2, 0.2)), 0.5, 2.0),
        "norm_gain": jnp.clip(1.0 + 0.18 * jax.random.normal(streams_of[7], (LAYERS, D), jnp.float32), 0.1, 1.9),
        "conv_taps": normal_values(streams_of[8], (LAYERS, KERNEL, FF), 0.6, 3.0, ((2, 8),), jnp.float32),
        "conv_bias": normal_values(streams_of[9], (LAYERS, FF), 0.5, 3.0, ((1, 8),), jnp.float32),
    }


norm_eps = 1e-06
residual_scale = 0.25

def reference(tokens, gate_weight, up_weight, down_weight, gate_scale, up_scale, down_scale, norm_gain, conv_taps, conv_bias):
    hstate = tokens
    for layer in range(LAYERS):
        wide = hstate.astype(jnp.float32)
        stat = lax.optimization_barrier(jnp.mean(wide * wide, axis=1, keepdims=True))
        rscale = lax.rsqrt(stat + norm_eps)
        operand = (wide * norm_gain[layer]).astype(jnp.bfloat16)
        gate = jnp.dot(operand, gate_weight[layer].astype(jnp.bfloat16), preferred_element_type=jnp.float32) * rscale * gate_scale[layer]
        upward = jnp.dot(operand, up_weight[layer].astype(jnp.bfloat16), preferred_element_type=jnp.float32) * rscale * up_scale[layer]
        taps = conv_taps[layer]
        padded = jnp.pad(gate, ((1, 1), (0, 0)))
        mixed = taps[0] * padded[:-2] + taps[1] * padded[1:-1] + taps[2] * padded[2:] + conv_bias[layer]
        hidden = (jax.nn.silu(mixed) * upward).astype(jnp.bfloat16)
        branch = jnp.dot(hidden, down_weight[layer].astype(jnp.bfloat16), preferred_element_type=jnp.float32) * down_scale[layer]
        hstate = (residual_scale * wide + branch).astype(jnp.bfloat16)
    return hstate
```

```python
import functools

import jax
import jax.numpy as jnp
from jax import lax
from jax.experimental import pallas as pl
from jax.experimental.pallas import tpu as pltpu
from jax.sharding import PartitionSpec as P

MESH = pl.DeviceIdType.MESH
norm_eps = 1e-06
residual_scale = 0.25
LANES = 128
PACK = 16
CHUNKS = 4
LAG = 2
STAGES = "GABHIFJDZEWNR"


def row_chunks(n_tok, layers):
    step, shift = n_tok // CHUNKS, 4 * PACK
    chunks = []
    for l in range(layers):
        ends = [e - l * shift for e in range(step, n_tok + 1, step)]
        ends = [e for e in ends if 0 < e < n_tok] + [n_tok]
        chunks.append(list(zip([0] + ends[:-1], ends)))
    return chunks


def plan(chunks):
    n_tok, layers = chunks[0][-1][1], len(chunks)
    near, side, far = 1.0, 2.1, 2.9
    link = {"x": 0.0, "y": 0.0, "z": 0.0}
    cost = {
        "G": (1.0, 1.4), "A": (0.1, 0.15), "B": (0.1, 0.15), "H": (0.1, 0.2), "I": (0.1, 0.2), "F": (0.1, 0.0),
        "J": (0.1, 0.0), "D": (0.35, 0.65), "Z": (0.1, 0.1), "E": (0.1, 0.1), "W": (0.1, 0.0), "N": (0.1, 0.25),
        "R": (0.2, 0.1),
    }
    done, arrive, order, now = {}, {}, [], 0.0
    todo = [(l, k, s) for l in range(layers) for k in range(len(chunks[l])) for s in STAGES]
    todo = [o for o in todo if not (o[0] == layers - 1 and o[2] == "R")]

    def send(name, start, length, delay):
        begin = max(link[name], start)
        link[name] = begin + length
        return begin + length + delay

    def ready(l, k, s):
        needs = []
        if s == "G":
            if k > 0:
                needs.append((l, k - 1, "G"))
            if l > 0:
                last = min(chunks[l][k][1] + PACK, n_tok)
                needs += [(l - 1, j, "R") for j, (a, _) in enumerate(chunks[l - 1]) if a < last]
        else:
            needs.append((l, k, STAGES[STAGES.index(s) - 1]))
            if s == "A" and k > 0:
                needs.append((l, k - 1, "B"))
            if s == "B" and k > 0:
                needs.append((l, k - 1, "I"))
            if s == "N" and k + 1 < len(chunks[l]):
                needs.append((l, k + 1, "G"))
        if any(o not in done for o in needs):
            return None
        return max([0.0] + [done[o] for o in needs] + [arrive.get((l, k, s), 0.0)])

    while todo:
        best = None
        for o in todo:
            at = ready(*o)
            if at is not None:
                rank = (round(max(now, at), 1), o[0], o[1], STAGES.index(o[2]))
                if best is None or rank < best[0]:
                    best = (rank, o, max(now, at))
        _, o, start = best
        l, k, s = o
        q = (chunks[l][k][1] - chunks[l][k][0]) / 128
        now = start + cost[s][0] + cost[s][1] * q
        done[o] = now
        todo.remove(o)
        order.append(o)
        if s == "G":
            arrive[l, k, "A"] = now + near
        if s == "A":
            arrive[l, k, "H"] = send("x", start, 1.93 * q, side)
        if s == "B":
            arrive[l, k, "I"] = send("x", start, 1.93 * q, side)
        if s == "H":
            arrive[l, k, "F"] = send("x", start, 0.97 * q, side)
        if s == "I":
            arrive[l, k, "J"] = send("x", start, 0.97 * q, side)
        if s == "J":
            arrive[l, k, "D"] = now + near
        if s == "D":
            arrive[l, k, "E"] = send("y", now, 2.8 * q, side)
            arrive[l, k, "Z"] = arrive[l, k, "E"] - 2.1 * q
        if s == "Z":
            arrive[l, k, "E"] = max(send("z", start, 2.8 * q, far), arrive[l, k, "E"] + far)
        if s == "E":
            arrive[l, k, "N"] = send("z", now, 2.8 * q, far)
            arrive[l, k, "W"] = arrive[l, k, "N"] - 1.4 * q
        if s == "W":
            arrive[l, k, "N"] = max(send("y", start, 2.8 * q, side), arrive[l, k, "N"] + side)
        if s == "N":
            arrive[l, k, "R"] = now + side
    return order, now


def kernel(
    sizes,
    tok,
    gw_hbm,
    uw_hbm,
    dw_hbm,
    gs,
    us,
    ds_,
    gain,
    taps,
    bias,
    out,
    gw,
    uw,
    dw,
    dwb,
    operand,
    rsb,
    stat,
    part,
    crecv,
    xsend,
    xrecv,
    hid,
    ysend,
    own,
    yrecv,
    zsend,
    zrecv,
    hnew,
    wsem,
    lsem,
    ssem,
    csem,
    xsem,
    hsem,
    ysem,
    zsem,
    asem,
    fsem,
):
    chunks, n_tok, d_loc, f_loc, d_all, n_z = sizes
    layers = len(chunks)
    tiles = f_loc // LANES
    units = (tiles + 1) // 2
    pairs = tiles // 2
    piece, d_half = d_loc // (2 * n_z), d_loc // 2
    first = [sum(len(c) for c in chunks[:l]) for l in range(layers)]
    f32, bf16 = jnp.float32, jnp.bfloat16
    ra, cb = lax.axis_index("ra"), lax.axis_index("cb")
    z, y = ra // 2, ra % 2
    x, c = cb // 2, cb % 2
    core_dev = (ra, x * 2 + (1 - c))
    x_dev = (ra, (1 - x) * 2 + c)
    y_dev = (z * 2 + (1 - y), cb)

    def z_dev(i):
        return (lax.rem(z + i, n_z) * 2 + y, cb)

    def remote(src, dst, sems, dev):
        return pltpu.make_async_remote_copy(
            src_ref=src, dst_ref=dst, send_sem=sems[0], recv_sem=sems[1], device_id=dev, device_id_type=MESH
        )

    def span_of(at, width, size=1):
        return pl.ds(pl.multiple_of(at * width, width), size * width)

    def each(fn, begin=0, end=units):
        stop = min(end, pairs)
        if stop > begin:

            def step(u, carry):
                fn(u, 2)
                return carry

            lax.fori_loop(begin, stop, step, 0)
        if end > pairs:
            fn(pairs, 1)

    def first_load(u, w, n):
        src, dst = ((gw_hbm, gw), (uw_hbm, uw))[n]
        cols = span_of(u * 2, LANES, w)
        return pltpu.make_async_copy(src.at[0, :, cols], dst.at[0, :, cols], wsem.at[u, n])

    def load(l, n):
        src, dst = ((gw_hbm, gw), (uw_hbm, uw), (dw_hbm, dw))[n]
        return pltpu.make_async_copy(src.at[l], dst if n == 2 else dst.at[l], lsem.at[l, n])

    def start_first(u, w):
        first_load(u, w, 0).start()
        first_load(u, w, 1).start()

    each(start_first)

    barrier = pltpu.get_barrier_semaphore()
    peers = [(ra, lax.rem(cb + k, 4)) for k in range(1, 4)] + [y_dev] + [z_dev(k) for k in range(1, n_z)]
    for dev in peers:
        pl.semaphore_signal(barrier, inc=1, device_id=dev, device_id_type=MESH)
    pl.semaphore_wait(barrier, len(peers))

    def stat_copy(n, k):
        return remote(stat.at[n, 0], stat.at[n, k], (ssem.at[0, n, k - 1], ssem.at[1, n, k - 1]), (ra, lax.rem(cb + k, 4)))

    def picked(s, e):
        lane = lax.broadcasted_iota(jnp.int32, (e - s, LANES), 1)
        row = lax.broadcasted_iota(jnp.int32, (e - s, LANES), 0)
        return lane == lax.shift_right_logical(row + s, 3)

    def squares(n, h, l, s, e):
        wide = h[s:e, :].astype(f32)
        ssq = jnp.sum(wide * wide, axis=1, keepdims=True)
        packed = jnp.where(picked(s, e), jnp.broadcast_to(ssq, (e - s, LANES)), 0.0)
        stat[n, 0] = jnp.sum(packed.reshape((e - s) // 8, 8, LANES), axis=0)
        for k in range(1, 4):
            stat_copy(n, k).start()
        operand[s:e, :] = (wide * gain[l : l + 1, :]).astype(bf16)

    def scale_rows(n, s, e):
        for k in range(1, 4):
            stat_copy(n, k).wait()
        total = stat[n, 0] + stat[n, 1] + stat[n, 2] + stat[n, 3]
        spread = jnp.broadcast_to(total[None], ((e - s) // 8, 8, LANES)).reshape(e - s, LANES)
        summed = jnp.sum(jnp.where(picked(s, e), spread, 0.0), axis=1, keepdims=True)
        rsb[s:e, :] = jnp.broadcast_to(lax.rsqrt(summed / d_all + norm_eps), (e - s, LANES))

    def steps_of(l, k):
        s, e = chunks[l][k]
        at = first[l] + k
        half, quarter = (e - s) // 2, (e - s) // 4
        lo, hi = max(s - PACK, 0), min(e + PACK, n_tok)
        h = tok if l == 0 else hnew.at[l - 1]

        def block_rows(cc, xx):
            return pl.ds(pl.multiple_of(s + cc * half + xx * quarter, PACK), quarter)

        def local_rows(xx):
            return pl.ds(pl.multiple_of(s // 2 + xx * quarter, PACK), quarter)

        x_rows = slice(s // 4, e // 4)

        def core_copy(u, w):
            rows = pl.ds(pl.multiple_of(s + (1 - c) * half, PACK), half)
            cols = span_of(u * 4, LANES, 2 * w)
            dst = crecv.at[l, s // 2 : e // 2, cols]
            return remote(part.at[rows, cols], dst, (csem.at[0, at, u], csem.at[1, at, u]), core_dev)

        def x_copy(u, w):
            cols = span_of(u * 4, LANES, 2 * w)
            sems = (xsem.at[0, at, u], xsem.at[1, at, u])
            return remote(xsend.at[x_rows, cols], xrecv.at[l, x_rows, cols], sems, x_dev)

        def h_copy(u, w, n):
            cols = span_of(u * 2, LANES, w)
            block = hid.at[l, block_rows(c, 1 - x if n == 2 else x), cols]
            return remote(block, block, (hsem.at[0, at, n, u], hsem.at[1, at, n, u]), x_dev if n == 0 else core_dev)

        def y_copy(i):
            cols = span_of(lax.rem(z + i, n_z), piece)
            sems = (ysem.at[0, at, i - 1], ysem.at[1, at, i - 1])
            return remote(ysend.at[s:e, cols], yrecv.at[l, s:e, cols], sems, y_dev)

        def z_copy(i):
            cols = span_of(lax.rem(z + i, n_z), piece)
            sems = (zsem.at[0, at, i - 1], zsem.at[1, at, i - 1])
            return remote(zsend.at[s:e, cols], zrecv.at[l, i - 1, s:e, :], sems, z_dev(i))

        def gather_z(i):
            block = hnew.at[l, s:e, span_of(y * n_z + z, piece)]
            return remote(block, block, (asem.at[0, at, i - 1], asem.at[1, at, i - 1]), z_dev(i))

        def gather_y(i):
            block = hnew.at[l, s:e, span_of(y * n_z + lax.rem(z + n_z - i, n_z), piece)]
            return remote(block, block, (fsem.at[0, at, i], fsem.at[1, at, i]), y_dev)

        def gate_unit(u, w):
            if l == 0 and k == 0:
                first_load(u, w, 0).wait()
                first_load(u, w, 1).wait()
            cols = span_of(u * 2, LANES, w)
            weights = jnp.concatenate([gw[l, :, cols].astype(bf16), uw[l, :, cols].astype(bf16)], axis=1)
            acc = jnp.dot(operand[lo:hi, :], weights, preferred_element_type=f32)
            rs = rsb[lo:hi, :]
            rows = lax.broadcasted_iota(jnp.int32, rs.shape, 0)
            for i in range(w):
                col = span_of(u * 2 + i, LANES)
                g = acc[:, i * LANES : (i + 1) * LANES] * rs * gs[l : l + 1, col]
                prev, nxt = pltpu.roll(g, 1, 0), pltpu.roll(g, hi - lo - 1, 0)
                if s == 0:
                    prev = jnp.where(rows == 0, 0.0, prev)
                if e == n_tok:
                    nxt = jnp.where(rows == hi - lo - 1, 0.0, nxt)
                mixed = taps[l, 0:1, col] * prev + taps[l, 1:2, col] * g + taps[l, 2:3, col] * nxt
                upward = acc[:, (w + i) * LANES : (w + i + 1) * LANES] * rs * us[l : l + 1, col]
                part[s:e, span_of(u * 4 + 2 * i, LANES)] = mixed[s - lo : e - lo].astype(bf16)
                part[s:e, span_of(u * 4 + 2 * i + 1, LANES)] = upward[s - lo : e - lo].astype(bf16)
            core_copy(u, w).start()

        def x_unit(u, w):
            core_copy(u, w).wait_recv()
            cols = span_of(u * 4, LANES, 2 * w)
            mine = part[block_rows(c, 1 - x), cols].astype(f32)
            xsend[x_rows, cols] = (mine + crecv[l, local_rows(1 - x), cols].astype(f32)).astype(bf16)
            x_copy(u, w).start()

        def hidden_unit(u, w):
            x_copy(u, w).wait_recv()
            cols = span_of(u * 4, LANES, 2 * w)
            rows = block_rows(c, x)
            total = (
                part[rows, cols].astype(f32)
                + crecv[l, local_rows(x), cols].astype(f32)
                + xrecv[l, x_rows, cols].astype(f32)
            )
            for i in range(w):
                col = span_of(u * 2 + i, LANES)
                mixed = total[:, 2 * i * LANES : (2 * i + 1) * LANES] + bias[l : l + 1, col]
                upward = total[:, (2 * i + 1) * LANES : (2 * i + 2) * LANES]
                hid[l, rows, col] = (mixed / (1.0 + jnp.exp(-mixed)) * upward).astype(bf16)
            h_copy(u, w, 0).start()
            h_copy(u, w, 1).start()

        def forward_unit(u, w):
            h_copy(u, w, 0).wait_recv()
            h_copy(u, w, 2).start()

        def gathered_unit(u, w):
            h_copy(u, w, 1).wait_recv()
            h_copy(u, w, 2).wait_recv()

        middle = units // 2

        def gate():
            each(gate_unit)

        def gate_first():
            def step(u, carry):
                gate_unit(u, 2)

                @pl.when(u >= LAG)
                def _():
                    x_unit(u - LAG, 2)

                return carry

            lax.fori_loop(0, pairs, step, 0)
            if units > pairs:
                gate_unit(pairs, 1)
            each(x_unit, max(pairs - LAG, 0))

        def down():
            each(gathered_unit)
            rows = hid[l, s:e, :]
            other = jnp.dot(rows, dwb[l, :, span_of(1 - y, d_half)], preferred_element_type=f32)
            ysend[s:e, :] = other.astype(bf16)
            for i in range(1, n_z + 1):
                y_copy(i).start()
            own[s:e, :] = jnp.dot(rows, dwb[l, :, span_of(y, d_half)], preferred_element_type=f32)

        def spread():
            for i in range(1, n_z):
                cols = span_of(lax.rem(z + i, n_z), piece)
                y_copy(i).wait_recv()
                zsend[s:e, cols] = (own[s:e, cols] + yrecv[l, s:e, cols].astype(f32)).astype(bf16)
                z_copy(i).start()

        def finish():
            cols, mine = span_of(z, piece), span_of(y * n_z + z, piece)
            y_copy(n_z).wait_recv()
            acc = own[s:e, cols] + yrecv[l, s:e, cols].astype(f32)
            for i in range(1, n_z):
                z_copy(i).wait_recv()
                acc = acc + zrecv[l, i - 1, s:e, :].astype(f32)
            new = residual_scale * h[s:e, mine].astype(f32) + acc * ds_[l : l + 1, mine]
            hnew[l, s:e, mine] = new.astype(bf16)
            for i in range(1, n_z):
                gather_z(i).start()
            gather_y(0).start()

        def forward():
            for i in range(1, n_z):
                gather_z(i).wait_recv()
                gather_y(i).start()

        def sent_unit(u, w):
            core_copy(u, w).wait_send()
            x_copy(u, w).wait_send()
            for n in range(3):
                h_copy(u, w, n).wait_send()

        def arrived():
            for i in range(n_z):
                gather_y(i).wait_recv()
            if l + 1 < layers:
                squares(1 + at, hnew.at[l], l + 1, s, e)
            else:
                out[s:e, :] = hnew[l, s:e, :]
            each(sent_unit)
            for i in range(1, n_z + 1):
                y_copy(i).wait_send()
            for i in range(1, n_z):
                z_copy(i).wait_send()

        def sent():
            for i in range(1, n_z):
                gather_z(i).wait_send()
            for i in range(n_z):
                gather_y(i).wait_send()

        return {
            "G": gate_first if k == 0 else gate,
            "A": functools.partial(each, x_unit, 0, middle),
            "B": functools.partial(each, x_unit, middle),
            "H": functools.partial(each, hidden_unit, 0, middle),
            "I": functools.partial(each, hidden_unit, middle),
            "F": functools.partial(each, forward_unit, 0, middle),
            "J": functools.partial(each, forward_unit, middle),
            "D": down,
            "Z": spread,
            "E": finish,
            "W": forward,
            "N": arrived,
            "R": functools.partial(scale_rows, 1 + at, s, e),
            "sent": sent,
        }

    def cast_down(l):
        load(l, 2).wait()

        def step(i, carry):
            r = span_of(i, LANES)
            dwb[l, r, :] = dw[r, :].astype(bf16)
            return carry

        lax.fori_loop(0, tiles, step, 0)
        if l + 1 < layers:
            load(l + 1, 2).start()

    squares(0, tok, 0, 0, n_tok)
    scale_rows(0, 0, n_tok)
    steps = {(l, k): steps_of(l, k) for l in range(layers) for k in range(len(chunks[l]))}
    for l, k, s in plan(chunks)[0]:
        if s == "G" and l > 0 and k == 0:
            load(l, 0).wait()
            load(l, 1).wait()
        if s == "H" and (l, k) == (0, 0):
            cast_down(0)
        if s == "E" and k == 0 and l + 1 < layers:
            cast_down(l + 1)
        if k == 0 and s in "AB":
            continue
        steps[l, k][s]()
        if s == "G" and (l, k) == (0, 0):
            load(0, 2).start()
            for ll in range(1, layers):
                load(ll, 0).start()
                load(ll, 1).start()
    for group in steps.values():
        group["sent"]()


def fused(n_ra, tokens, gate_weight, up_weight, down_weight, gate_scale, up_scale, down_scale, gain, taps, bias, d_all):
    n_tok, d_loc = tokens.shape
    layers, _, f_loc = gate_weight.shape
    n_z = n_ra // 2
    chunks = row_chunks(n_tok, layers)
    total = sum(len(c) for c in chunks)
    tiles = f_loc // LANES
    units = (tiles + 1) // 2
    f32, bf16 = jnp.float32, jnp.bfloat16
    dma = pltpu.SemaphoreType.DMA
    vmem, hbm = pl.BlockSpec(memory_space=pltpu.VMEM), pl.BlockSpec(memory_space=pl.ANY)
    return pl.pallas_call(
        functools.partial(kernel, (chunks, n_tok, d_loc, f_loc, d_all, n_z)),
        out_shape=jax.ShapeDtypeStruct((n_tok, d_loc), bf16),
        in_specs=[vmem, hbm, hbm, hbm] + [vmem] * 6,
        out_specs=vmem,
        scratch_shapes=[
            pltpu.VMEM((layers, d_loc, f_loc), f32),
            pltpu.VMEM((layers, d_loc, f_loc), f32),
            pltpu.VMEM((f_loc, d_loc), f32),
            pltpu.VMEM((layers, f_loc, d_loc), bf16),
            pltpu.VMEM((n_tok, d_loc), bf16),
            pltpu.VMEM((n_tok, LANES), f32),
            pltpu.VMEM((1 + total, 4, 8, LANES), f32),
            pltpu.VMEM((n_tok, 2 * f_loc), bf16),
            pltpu.VMEM((layers, n_tok // 2, 2 * f_loc), bf16),
            pltpu.VMEM((n_tok // 4, 2 * f_loc), bf16),
            pltpu.VMEM((layers, n_tok // 4, 2 * f_loc), bf16),
            pltpu.VMEM((layers, n_tok, f_loc), bf16),
            pltpu.VMEM((n_tok, d_loc // 2), bf16),
            pltpu.VMEM((n_tok, d_loc // 2), f32),
            pltpu.VMEM((layers, n_tok, d_loc // 2), bf16),
            pltpu.VMEM((n_tok, d_loc // 2), bf16),
            pltpu.VMEM((layers, n_z - 1, n_tok, d_loc // n_ra), bf16),
            pltpu.VMEM((layers, n_tok, d_loc), bf16),
            dma((units, 2)),
            dma((layers, 3)),
            dma((2, 1 + total, 3)),
            dma((2, total, units)),
            dma((2, total, units)),
            dma((2, total, 3, units)),
            dma((2, total, n_z)),
            dma((2, total, n_z - 1)),
            dma((2, total, n_z - 1)),
            dma((2, total, n_z)),
        ],
        compiler_params=pltpu.CompilerParams(
            collective_id=0, has_side_effects=True, vmem_limit_bytes=67_043_328
        ),
    )(tokens, gate_weight, up_weight, down_weight, gate_scale, up_scale, down_scale, gain, taps, bias)


def plain(tokens, gate_weight, up_weight, down_weight, gate_scale, up_scale, down_scale, gain, conv_taps, bias, d_all):
    hstate = tokens
    for layer in range(gate_weight.shape[0]):
        wide = hstate.astype(jnp.float32)
        squares = jnp.sum(wide * wide, axis=1)
        operand = (wide * gain[layer]).astype(jnp.bfloat16)
        gate_part = jnp.dot(operand, gate_weight[layer].astype(jnp.bfloat16), preferred_element_type=jnp.float32)
        up_part = jnp.dot(operand, up_weight[layer].astype(jnp.bfloat16), preferred_element_type=jnp.float32)
        gate_sum, up_sum, square_sum = lax.psum((gate_part, up_part, squares), "cb")
        rscale = lax.rsqrt(square_sum / d_all + norm_eps)[:, None]
        gate = gate_sum * rscale * gate_scale[layer]
        upward = up_sum * rscale * up_scale[layer]
        padded = jnp.pad(gate, ((1, 1), (0, 0)))
        taps = conv_taps[layer]
        mixed = taps[0] * padded[:-2] + taps[1] * padded[1:-1] + taps[2] * padded[2:] + bias[layer]
        hidden = (jax.nn.silu(mixed) * upward).astype(jnp.bfloat16)
        term = jnp.dot(hidden, down_weight[layer].astype(jnp.bfloat16), preferred_element_type=jnp.float32)
        branch = lax.psum(term, "ra") * down_scale[layer]
        hstate = (residual_scale * wide + branch).astype(jnp.bfloat16)
    return hstate


def solution(mesh):
    n_ra, n_cb = mesh.shape["ra"], mesh.shape["cb"]

    def per_device(*args):
        n_tok, d_loc = args[0].shape
        f_loc = args[1].shape[2]
        fits = n_cb == 4 and n_ra % 2 == 0 and n_ra >= 4 and n_tok % (4 * PACK * CHUNKS) == 0 and n_tok <= 8 * LANES
        fits = fits and f_loc % LANES == 0 and d_loc % (LANES * n_ra) == 0 and f_loc >= 2 * LAG * LANES
        if fits:
            return fused(n_ra, *args, d_loc * n_cb)
        return plain(*args, d_loc * n_cb)

    in_specs = (
        P(None, "cb"),
        P(None, "cb", "ra"),
        P(None, "cb", "ra"),
        P(None, "ra", "cb"),
        P(None, "ra"),
        P(None, "ra"),
        P(None, "cb"),
        P(None, "cb"),
        P(None, None, "ra"),
        P(None, "ra"),
    )
    return jax.shard_map(
        per_device, mesh=mesh, in_specs=in_specs, out_specs=P(None, "cb"), check_vma=False
    )
```

```python
import functools

import jax
import jax.numpy as jnp
from jax import lax
from jax.experimental import pallas as pl
from jax.experimental.pallas import tpu as pltpu
from jax.sharding import PartitionSpec as P

MESH = pl.DeviceIdType.MESH
norm_eps = 1e-06
residual_scale = 0.25
LANES = 128
PACK = 16


ENDS = ((2, 3, 4, 6, 7, 8), (1, 2, 3, 5, 7, 8))


def row_chunks(n_tok):
    return [[(a * n_tok // 8, b * n_tok // 8) for a, b in zip((0,) + ends[:-1], ends)] for ends in ENDS]


ORDER = (
    ("M", 0, 0), ("G", 0, 0), ("K", 0, 0), ("A", 0, 0), ("B", 0, 0), ("G", 0, 1), ("K", 0, 1), ("G", 0, 2),
    ("C", 0, 0), ("A", 0, 1), ("K", 0, 2), ("H", 0, 0), ("B", 0, 1), ("G", 0, 3), ("I", 0, 0), ("A", 0, 2),
    ("H", 0, 1), ("K", 0, 3), ("F", 0, 0), ("B", 0, 2), ("G", 0, 4), ("J", 0, 0), ("I", 0, 1), ("A", 0, 3),
    ("D", 0, 0), ("H", 0, 2), ("F", 0, 1), ("B", 0, 3), ("K", 0, 4), ("J", 0, 1), ("A", 0, 4), ("I", 0, 2),
    ("G", 0, 5), ("D", 0, 1), ("F", 0, 2), ("Z", 0, 0), ("H", 0, 3), ("I", 0, 3), ("A", 0, 5), ("K", 0, 5),
    ("Z", 0, 1), ("J", 0, 2), ("F", 0, 3), ("B", 0, 4), ("B", 0, 5), ("C", 1, 0), ("D", 0, 2), ("J", 0, 3),
    ("E", 0, 0), ("H", 0, 5), ("D", 0, 3), ("E", 0, 1), ("H", 0, 4), ("I", 0, 5), ("Z", 0, 2), ("F", 0, 5),
    ("I", 0, 4), ("W", 0, 0), ("J", 0, 5), ("Z", 0, 3), ("D", 0, 5), ("F", 0, 4), ("J", 0, 4), ("W", 0, 1),
    ("E", 0, 2), ("D", 0, 4), ("N", 0, 0), ("Z", 0, 5), ("E", 0, 3), ("M", 1, 0), ("W", 0, 2), ("R", 0, 0),
    ("Z", 0, 4), ("G", 1, 0), ("N", 0, 1), ("K", 1, 0), ("A", 1, 0), ("N", 0, 2), ("E", 0, 5), ("R", 0, 1),
    ("B", 1, 0), ("W", 0, 3), ("G", 1, 1), ("K", 1, 1), ("E", 0, 4), ("A", 1, 1), ("R", 0, 2), ("G", 1, 2),
    ("H", 1, 0), ("W", 0, 5), ("I", 1, 0), ("N", 0, 3), ("A", 1, 2), ("K", 1, 2), ("B", 1, 1), ("W", 0, 4),
    ("F", 1, 0), ("H", 1, 1), ("B", 1, 2), ("N", 0, 5), ("R", 0, 3), ("G", 1, 3), ("J", 1, 0), ("H", 1, 2),
    ("N", 0, 4), ("A", 1, 3), ("K", 1, 3), ("R", 0, 5), ("I", 1, 2), ("F", 1, 2), ("F", 1, 1), ("I", 1, 1),
    ("B", 1, 3), ("R", 0, 4), ("G", 1, 4), ("K", 1, 4), ("A", 1, 4), ("J", 1, 2), ("D", 1, 0), ("H", 1, 3),
    ("B", 1, 4), ("D", 1, 2), ("J", 1, 1), ("D", 1, 1), ("Z", 1, 0), ("I", 1, 3), ("G", 1, 5), ("H", 1, 4),
    ("F", 1, 3), ("Z", 1, 2), ("K", 1, 5), ("I", 1, 4), ("A", 1, 5), ("Z", 1, 1), ("J", 1, 3), ("E", 1, 0),
    ("F", 1, 4), ("B", 1, 5), ("D", 1, 3), ("E", 1, 2), ("J", 1, 4), ("E", 1, 1), ("H", 1, 5), ("D", 1, 4),
    ("I", 1, 5), ("Z", 1, 3), ("F", 1, 5), ("W", 1, 1), ("Z", 1, 4), ("W", 1, 2), ("J", 1, 5), ("D", 1, 5),
    ("E", 1, 3), ("W", 1, 0), ("N", 1, 1), ("Z", 1, 5), ("E", 1, 4), ("W", 1, 3), ("E", 1, 5), ("N", 1, 2),
    ("W", 1, 4), ("W", 1, 5), ("N", 1, 4), ("N", 1, 3), ("N", 1, 0), ("N", 1, 5),
)

def kernel(
    sizes,
    tok,
    gw_hbm,
    uw_hbm,
    dw_hbm,
    gs,
    us,
    ds_,
    gain,
    taps,
    bias,
    out,
    gw,
    uw,
    dw,
    dwb,
    operand,
    rsb,
    stat,
    part,
    crecv,
    xsend,
    xrecv,
    hid,
    ysend,
    own,
    yrecv,
    zsend,
    zrecv,
    hnew,
    raw,
    wsem,
    lsem,
    ssem,
    sent,
    csem,
    xsem,
    hsem,
    osem,
    ysem,
    zsem,
    asem,
    fsem,
):
    chunks, n_tok, d_loc, f_loc, d_all, n_z = sizes
    layers = len(chunks)
    tiles = f_loc // LANES
    units = (tiles + 1) // 2
    pairs, middle = tiles // 2, units // 2
    piece, d_half = d_loc // (2 * n_z), d_loc // 2
    first = [sum(len(c) for c in chunks[:l]) for l in range(layers)]
    f32, bf16 = jnp.float32, jnp.bfloat16
    ra, cb = lax.axis_index("ra"), lax.axis_index("cb")
    z, y = ra // 2, ra % 2
    x, c = cb // 2, cb % 2
    core_dev = (ra, x * 2 + (1 - c))
    x_dev = (ra, (1 - x) * 2 + c)
    y_dev = (z * 2 + (1 - y), cb)

    def z_dev(i):
        return (lax.rem(z + i, n_z) * 2 + y, cb)

    def remote(src, dst, sems, dev):
        return pltpu.make_async_remote_copy(
            src_ref=src, dst_ref=dst, send_sem=sems[0], recv_sem=sems[1], device_id=dev, device_id_type=MESH
        )

    def span_of(at, width, size=1):
        return pl.ds(pl.multiple_of(at * width, width), size * width)

    def each(fn, begin=0, end=units):
        stop = min(end, pairs)
        if stop > begin:

            def step(u, carry):
                fn(u, 2)
                return carry

            lax.fori_loop(begin, stop, step, 0)
        if end > pairs:
            fn(pairs, 1)

    def first_load(u, w, n):
        src, dst = ((gw_hbm, gw), (uw_hbm, uw))[n]
        cols = span_of(u * 2, LANES, w)
        return pltpu.make_async_copy(src.at[0, :, cols], dst.at[0, :, cols], wsem.at[u, n])

    def load(l, n):
        src, dst = ((gw_hbm, gw), (uw_hbm, uw), (dw_hbm, dw))[n]
        return pltpu.make_async_copy(src.at[l], dst if n == 2 else dst.at[l], lsem.at[l, n])

    def start_first(u, w):
        first_load(u, w, 0).start()
        first_load(u, w, 1).start()

    each(start_first)

    def stat_copy(n, k):
        return remote(stat.at[n, 0], stat.at[n, k], (ssem.at[0, n], ssem.at[1, n]), (ra, lax.rem(cb + k, 4)))

    def picked(s, e):
        lane = lax.broadcasted_iota(jnp.int32, (e - s, LANES), 1)
        row = lax.broadcasted_iota(jnp.int32, (e - s, LANES), 0)
        return lane == lax.shift_right_logical(row + s, 3)

    def squares(n, h, l, s, e):
        wide = h[s:e, :].astype(f32)
        ssq = jnp.sum(wide * wide, axis=1, keepdims=True)
        packed = jnp.where(picked(s, e), jnp.broadcast_to(ssq, (e - s, LANES)), 0.0)
        stat[n, 0] = jnp.sum(packed.reshape((e - s) // 8, 8, LANES), axis=0)
        operand[s:e, :] = (wide * gain[l : l + 1, :]).astype(bf16)

    def share_squares(n):
        for k in range(1, 4):
            stat_copy(n, k).start()

    def scale_rows(n, s, e):
        others = stat.at[n, 1:4]
        remote(others, others, (ssem.at[0, n], ssem.at[1, n]), core_dev).wait()
        total = stat[n, 0] + stat[n, 1] + stat[n, 2] + stat[n, 3]
        spread = jnp.broadcast_to(total[None], ((e - s) // 8, 8, LANES)).reshape(e - s, LANES)
        summed = jnp.sum(jnp.where(picked(s, e), spread, 0.0), axis=1, keepdims=True)
        rsb[s:e, :] = jnp.broadcast_to(lax.rsqrt(summed / d_all + norm_eps), (e - s, LANES))

    def cast_down(l):
        load(l, 2).wait()

        def step(i, carry):
            r = span_of(i, LANES)
            dwb[l, r, :] = dw[r, :].astype(bf16)
            return carry

        lax.fori_loop(0, tiles, step, 0)
        if l + 1 < layers:
            load(l + 1, 2).start()

    def wait_sent(l, n):
        block = (
            part.at[0 : n_tok // 2, :],
            xsend,
            hid.at[l, 0 : 3 * n_tok // 4, :],
            ysend,
            zsend.at[:, 0 : (n_z - 1) * piece],
            hnew.at[l, :, 0 : (n_z - 1) * piece],
            hnew.at[l, :, 0:d_half],
        )[n]
        remote(block, block, (sent.at[l, n], csem.at[0, 0]), core_dev).wait_send()

    def steps_of(l, k):
        s, e = chunks[l][k]
        at = first[l] + k
        half, quarter = (e - s) // 2, (e - s) // 4
        lo, hi = max(s - PACK, 0), min(e + PACK, n_tok)
        h = tok if l == 0 else hnew.at[l - 1]

        def block_rows(cc, xx):
            return pl.ds(pl.multiple_of(s + cc * half + xx * quarter, PACK), quarter)

        def local_rows(xx):
            return pl.ds(pl.multiple_of(s // 2 + xx * quarter, PACK), quarter)

        x_rows = slice(s // 4, e // 4)

        def wide_cols(hf, width):
            return slice(0, middle * width) if hf == 0 else slice(middle * width, 2 * f_loc * width // (4 * LANES))

        def core_copy(hf):
            rows = pl.ds(pl.multiple_of(s + (1 - c) * half, PACK), half)
            cols = wide_cols(hf, 4 * LANES)
            return remote(part.at[rows, cols], crecv.at[l, s // 2 : e // 2, cols], (sent.at[l, 0], csem.at[at, hf]), core_dev)

        def x_copy(hf):
            cols = wide_cols(hf, 4 * LANES)
            return remote(xsend.at[x_rows, cols], xrecv.at[l, x_rows, cols], (sent.at[l, 1], xsem.at[at, hf]), x_dev)

        def h_copy(hf, n):
            block = hid.at[l, block_rows(c, 1 - x if n == 2 else x), wide_cols(hf, 2 * LANES)]
            return remote(block, block, (sent.at[l, 2], hsem.at[at, hf] if n == 0 else osem.at[at]), x_dev if n == 0 else core_dev)

        def y_copy(i):
            cols = span_of(lax.rem(z + i, n_z), piece)
            return remote(ysend.at[s:e, cols], yrecv.at[l, s:e, cols], (sent.at[l, 3], ysem.at[at, i - 1]), y_dev)

        def z_copy(i):
            cols = span_of(lax.rem(z + i, n_z), piece)
            return remote(zsend.at[s:e, cols], zrecv.at[l, i - 1, s:e, :], (sent.at[l, 4], zsem.at[at]), z_dev(i))

        def gather_z(i):
            block = hnew.at[l, s:e, span_of(y * n_z + z, piece)]
            return remote(block, block, (sent.at[l, 5], asem.at[at, i - 1]), z_dev(i))

        def gather_y(i):
            block = hnew.at[l, s:e, span_of(y * n_z + lax.rem(z + n_z - i, n_z), piece)]
            return remote(block, block, (sent.at[l, 6], fsem.at[at]), y_dev)

        def product(u, w):
            cols = span_of(u * 2, LANES, w)
            weights = jnp.concatenate([gw[l, :, cols].astype(bf16), uw[l, :, cols].astype(bf16)], axis=1)
            return jnp.dot(operand[lo:hi, :], weights, preferred_element_type=f32)

        def raw_unit(u, w):
            if l == 0:
                first_load(u, w, 0).wait()
                first_load(u, w, 1).wait()
            raw[0 : hi - lo, span_of(u * 4, LANES, 2 * w)] = product(u, w)

        def gate_unit(u, w):
            acc = raw[0 : hi - lo, span_of(u * 4, LANES, 2 * w)] if k == 0 else product(u, w)
            rs = rsb[lo:hi, :]
            rows = lax.broadcasted_iota(jnp.int32, rs.shape, 0)
            for i in range(w):
                col = span_of(u * 2 + i, LANES)
                g = acc[:, i * LANES : (i + 1) * LANES] * rs * gs[l : l + 1, col]
                prev, nxt = pltpu.roll(g, 1, 0), pltpu.roll(g, hi - lo - 1, 0)
                if s == 0:
                    prev = jnp.where(rows == 0, 0.0, prev)
                if e == n_tok:
                    nxt = jnp.where(rows == hi - lo - 1, 0.0, nxt)
                mixed = taps[0, l : l + 1, col] * prev + taps[1, l : l + 1, col] * g + taps[2, l : l + 1, col] * nxt
                upward = acc[:, (w + i) * LANES : (w + i + 1) * LANES] * rs * us[l : l + 1, col]
                part[s:e, span_of(u * 4 + 2 * i, LANES)] = mixed[s - lo : e - lo].astype(bf16)
                part[s:e, span_of(u * 4 + 2 * i + 1, LANES)] = upward[s - lo : e - lo].astype(bf16)

        def x_unit(u, w):
            cols = span_of(u * 4, LANES, 2 * w)
            mine = part[block_rows(c, 1 - x), cols].astype(f32)
            xsend[x_rows, cols] = (mine + crecv[l, local_rows(1 - x), cols].astype(f32)).astype(bf16)

        def hidden_unit(u, w):
            cols = span_of(u * 4, LANES, 2 * w)
            rows = block_rows(c, x)
            total = (
                part[rows, cols].astype(f32)
                + crecv[l, local_rows(x), cols].astype(f32)
                + xrecv[l, x_rows, cols].astype(f32)
            )
            for i in range(w):
                col = span_of(u * 2 + i, LANES)
                mixed = total[:, 2 * i * LANES : (2 * i + 1) * LANES] + bias[l : l + 1, col]
                upward = total[:, (2 * i + 1) * LANES : (2 * i + 2) * LANES]
                hid[l, rows, col] = (mixed / (1.0 + jnp.exp(-mixed)) * upward).astype(bf16)

        def bounds(hf):
            return (0, middle) if hf == 0 else (middle, units)

        def gate(hf):
            each(gate_unit, *bounds(hf))
            core_copy(hf).start()

        def reduce_x(hf):
            core_copy(hf).wait_recv()
            each(x_unit, *bounds(hf))
            x_copy(hf).start()

        def hidden(hf):
            x_copy(hf).wait_recv()
            each(hidden_unit, *bounds(hf))
            h_copy(hf, 0).start()
            h_copy(hf, 1).start()

        def forward_hidden(hf):
            h_copy(hf, 0).wait_recv()
            h_copy(hf, 2).start()

        def down():
            theirs = hid.at[l, pl.ds(pl.multiple_of(s + (1 - c) * half, PACK), half), :]
            remote(theirs, theirs, (sent.at[l, 2], osem.at[at]), core_dev).wait_recv()
            rows = hid[l, s:e, :]
            other = jnp.dot(rows, dwb[l, :, span_of(1 - y, d_half)], preferred_element_type=f32)
            ysend[s:e, :] = other.astype(bf16)
            for i in range(1, n_z + 1):
                y_copy(i).start()
            own[s:e, :] = jnp.dot(rows, dwb[l, :, span_of(y, d_half)], preferred_element_type=f32)

        def spread():
            for i in range(1, n_z):
                cols = span_of(lax.rem(z + i, n_z), piece)
                y_copy(i).wait_recv()
                zsend[s:e, cols] = (own[s:e, cols] + yrecv[l, s:e, cols].astype(f32)).astype(bf16)
                z_copy(i).start()

        def finish():
            cols, mine = span_of(z, piece), span_of(y * n_z + z, piece)
            y_copy(n_z).wait_recv()
            acc = own[s:e, cols] + yrecv[l, s:e, cols].astype(f32)
            pieces = zrecv.at[l, :, s:e, :]
            remote(pieces, pieces, (sent.at[l, 4], zsem.at[at]), y_dev).wait_recv()
            for i in range(1, n_z):
                acc = acc + zrecv[l, i - 1, s:e, :].astype(f32)
            new = residual_scale * h[s:e, mine].astype(f32) + acc * ds_[l : l + 1, mine]
            hnew[l, s:e, mine] = new.astype(bf16)
            for i in range(1, n_z):
                gather_z(i).start()
            gather_y(0).start()

        def forward():
            for i in range(1, n_z):
                gather_z(i).wait_recv()
                gather_y(i).start()

        def arrived():
            theirs = hnew.at[l, s:e, span_of(1 - y, d_half)]
            remote(theirs, theirs, (sent.at[l, 6], fsem.at[at]), y_dev).wait_recv()
            if l + 1 < layers:
                squares(1 + at, hnew.at[l], l + 1, s, e)
                share_squares(1 + at)
            else:
                out[s:e, :] = hnew[l, s:e, :]

        return {
            "M": functools.partial(each, raw_unit),
            "G": functools.partial(gate, 0),
            "K": functools.partial(gate, 1),
            "A": functools.partial(reduce_x, 0),
            "B": functools.partial(reduce_x, 1),
            "H": functools.partial(hidden, 0),
            "I": functools.partial(hidden, 1),
            "F": functools.partial(forward_hidden, 0),
            "J": functools.partial(forward_hidden, 1),
            "D": down,
            "Z": spread,
            "E": finish,
            "W": forward,
            "N": arrived,
            "R": functools.partial(scale_rows, 1 + at, s, e),
            "C": functools.partial(cast_down, l),
        }

    squares(0, tok, 0, 0, n_tok)
    barrier = pltpu.get_barrier_semaphore()
    peers = [(ra, lax.rem(cb + k, 4)) for k in range(1, 4)] + [y_dev] + [z_dev(k) for k in range(1, n_z)]
    for dev in peers:
        pl.semaphore_signal(barrier, inc=1, device_id=dev, device_id_type=MESH)
    pl.semaphore_wait(barrier, len(peers))

    share_squares(0)
    steps = {(l, k): steps_of(l, k) for l in range(layers) for k in range(len(chunks[l]))}
    begun = set()
    reused = {"G": 0, "A": 1, "D": 3, "Z": 4}
    for s, l, k in ORDER:
        if l > 0 and (s, l) not in begun and s in reused:
            wait_sent(l - 1, reused[s])
        begun.add((s, l))
        if s == "M" and l > 0:
            load(l, 0).wait()
            load(l, 1).wait()
        steps[l, k][s]()
        if (s, l) == ("M", 0):
            load(0, 2).start()
            for ll in range(1, layers):
                load(ll, 0).start()
                load(ll, 1).start()
            scale_rows(0, 0, n_tok)
    for l in range(layers):
        for n in range(7):
            if l == layers - 1 or n not in reused.values():
                wait_sent(l, n)


def fused(n_ra, tokens, gate_weight, up_weight, down_weight, gate_scale, up_scale, down_scale, gain, taps, bias, d_all):
    n_tok, d_loc = tokens.shape
    layers, _, f_loc = gate_weight.shape
    n_z = n_ra // 2
    chunks = row_chunks(n_tok)
    total = sum(len(c) for c in chunks)
    tiles = f_loc // LANES
    units = (tiles + 1) // 2
    f32, bf16 = jnp.float32, jnp.bfloat16
    dma = pltpu.SemaphoreType.DMA
    vmem, hbm = pl.BlockSpec(memory_space=pltpu.VMEM), pl.BlockSpec(memory_space=pl.ANY)
    return pl.pallas_call(
        functools.partial(kernel, (chunks, n_tok, d_loc, f_loc, d_all, n_z)),
        out_shape=jax.ShapeDtypeStruct((n_tok, d_loc), bf16),
        in_specs=[vmem, hbm, hbm, hbm] + [vmem] * 6,
        out_specs=vmem,
        scratch_shapes=[
            pltpu.VMEM((layers, d_loc, f_loc), f32),
            pltpu.VMEM((layers, d_loc, f_loc), f32),
            pltpu.VMEM((f_loc, d_loc), f32),
            pltpu.VMEM((layers, f_loc, d_loc), bf16),
            pltpu.VMEM((n_tok, d_loc), bf16),
            pltpu.VMEM((n_tok, LANES), f32),
            pltpu.VMEM((1 + total, 4, 8, LANES), f32),
            pltpu.VMEM((n_tok, 2 * f_loc), bf16),
            pltpu.VMEM((layers, n_tok // 2, 2 * f_loc), bf16),
            pltpu.VMEM((n_tok // 4, 2 * f_loc), bf16),
            pltpu.VMEM((layers, n_tok // 4, 2 * f_loc), bf16),
            pltpu.VMEM((layers, n_tok, f_loc), bf16),
            pltpu.VMEM((n_tok, d_loc // 2), bf16),
            pltpu.VMEM((n_tok, d_loc // 2), f32),
            pltpu.VMEM((layers, n_tok, d_loc // 2), bf16),
            pltpu.VMEM((n_tok, d_loc // 2), bf16),
            pltpu.VMEM((layers, n_z - 1, n_tok, d_loc // n_ra), bf16),
            pltpu.VMEM((layers, n_tok, d_loc), bf16),
            pltpu.VMEM((chunks[0][0][1] + PACK, 2 * f_loc), f32),
            dma((units, 2)),
            dma((layers, 3)),
            dma((2, 1 + total)),
            dma((layers, 7)),
            dma((total, 2)),
            dma((total, 2)),
            dma((total, 2)),
            dma((total,)),
            dma((total, n_z)),
            dma((total,)),
            dma((total, n_z - 1)),
            dma((total,)),
        ],
        compiler_params=pltpu.CompilerParams(
            collective_id=0, has_side_effects=True, vmem_limit_bytes=67_043_328
        ),
    )(tokens, gate_weight, up_weight, down_weight, gate_scale, up_scale, down_scale, gain, jnp.transpose(taps, (1, 0, 2)), bias)


def plain(tokens, gate_weight, up_weight, down_weight, gate_scale, up_scale, down_scale, gain, conv_taps, bias, d_all):
    hstate = tokens
    for layer in range(gate_weight.shape[0]):
        wide = hstate.astype(jnp.float32)
        squares = jnp.sum(wide * wide, axis=1)
        operand = (wide * gain[layer]).astype(jnp.bfloat16)
        gate_part = jnp.dot(operand, gate_weight[layer].astype(jnp.bfloat16), preferred_element_type=jnp.float32)
        up_part = jnp.dot(operand, up_weight[layer].astype(jnp.bfloat16), preferred_element_type=jnp.float32)
        gate_sum, up_sum, square_sum = lax.psum((gate_part, up_part, squares), "cb")
        rscale = lax.rsqrt(square_sum / d_all + norm_eps)[:, None]
        gate = gate_sum * rscale * gate_scale[layer]
        upward = up_sum * rscale * up_scale[layer]
        padded = jnp.pad(gate, ((1, 1), (0, 0)))
        taps = conv_taps[layer]
        mixed = taps[0] * padded[:-2] + taps[1] * padded[1:-1] + taps[2] * padded[2:] + bias[layer]
        hidden = (jax.nn.silu(mixed) * upward).astype(jnp.bfloat16)
        term = jnp.dot(hidden, down_weight[layer].astype(jnp.bfloat16), preferred_element_type=jnp.float32)
        branch = lax.psum(term, "ra") * down_scale[layer]
        hstate = (residual_scale * wide + branch).astype(jnp.bfloat16)
    return hstate


def solution(mesh):
    n_ra, n_cb = mesh.shape["ra"], mesh.shape["cb"]

    def per_device(*args):
        n_tok, d_loc = args[0].shape
        f_loc = args[1].shape[2]
        fits = n_cb == 4 and n_ra % 2 == 0 and n_ra >= 4 and n_tok % (8 * 4 * PACK) == 0 and n_tok <= 8 * LANES
        fits = fits and f_loc % LANES == 0 and d_loc % (LANES * n_ra) == 0 and f_loc >= 4 * LANES and args[1].shape[0] == len(ENDS)
        if fits:
            return fused(n_ra, *args, d_loc * n_cb)
        return plain(*args, d_loc * n_cb)

    in_specs = (
        P(None, "cb"),
        P(None, "cb", "ra"),
        P(None, "cb", "ra"),
        P(None, "ra", "cb"),
        P(None, "ra"),
        P(None, "ra"),
        P(None, "cb"),
        P(None, "cb"),
        P(None, None, "ra"),
        P(None, "ra"),
    )
    return jax.shard_map(
        per_device, mesh=mesh, in_specs=in_specs, out_specs=P(None, "cb"), check_vma=False
    )
```

```python
import functools

import jax
import jax.numpy as jnp
from jax import lax
from jax.experimental import pallas as pl
from jax.experimental.pallas import tpu as pltpu
from jax.sharding import PartitionSpec as P

MESH = pl.DeviceIdType.MESH
norm_eps = 1e-06
residual_scale = 0.25
LANES = 128
PACK = 16


ENDS = ((2, 3, 4, 6, 7, 8), (1, 2, 3, 5, 7, 8))


def row_chunks(n_tok):
    return [[(a * n_tok // 8, b * n_tok // 8) for a, b in zip((0,) + ends[:-1], ends)] for ends in ENDS]


ORDER = (
    ("M", 0, 0), ("G", 0, 0), ("K", 0, 0), ("A", 0, 0), ("B", 0, 0), ("G", 0, 1), ("K", 0, 1), ("G", 0, 2),
    ("C", 0, 0), ("A", 0, 1), ("K", 0, 2), ("H", 0, 0), ("B", 0, 1), ("G", 0, 3), ("I", 0, 0), ("A", 0, 2),
    ("H", 0, 1), ("K", 0, 3), ("F", 0, 0), ("B", 0, 2), ("G", 0, 4), ("J", 0, 0), ("I", 0, 1), ("A", 0, 3),
    ("D", 0, 0), ("H", 0, 2), ("F", 0, 1), ("B", 0, 3), ("K", 0, 4), ("J", 0, 1), ("A", 0, 4), ("I", 0, 2),
    ("G", 0, 5), ("D", 0, 1), ("F", 0, 2), ("Z", 0, 0), ("H", 0, 3), ("I", 0, 3), ("A", 0, 5), ("K", 0, 5),
    ("Z", 0, 1), ("J", 0, 2), ("F", 0, 3), ("B", 0, 4), ("B", 0, 5), ("C", 1, 0), ("D", 0, 2), ("J", 0, 3),
    ("E", 0, 0), ("H", 0, 5), ("D", 0, 3), ("E", 0, 1), ("H", 0, 4), ("I", 0, 5), ("Z", 0, 2), ("F", 0, 5),
    ("I", 0, 4), ("W", 0, 0), ("J", 0, 5), ("Z", 0, 3), ("D", 0, 5), ("F", 0, 4), ("J", 0, 4), ("W", 0, 1),
    ("E", 0, 2), ("D", 0, 4), ("N", 0, 0), ("Z", 0, 5), ("E", 0, 3), ("M", 1, 0), ("W", 0, 2), ("R", 0, 0),
    ("Z", 0, 4), ("G", 1, 0), ("N", 0, 1), ("K", 1, 0), ("A", 1, 0), ("N", 0, 2), ("E", 0, 5), ("R", 0, 1),
    ("B", 1, 0), ("W", 0, 3), ("G", 1, 1), ("K", 1, 1), ("E", 0, 4), ("A", 1, 1), ("R", 0, 2), ("G", 1, 2),
    ("H", 1, 0), ("W", 0, 5), ("I", 1, 0), ("N", 0, 3), ("A", 1, 2), ("K", 1, 2), ("B", 1, 1), ("W", 0, 4),
    ("F", 1, 0), ("H", 1, 1), ("B", 1, 2), ("N", 0, 5), ("R", 0, 3), ("G", 1, 3), ("J", 1, 0), ("H", 1, 2),
    ("N", 0, 4), ("A", 1, 3), ("K", 1, 3), ("R", 0, 5), ("I", 1, 2), ("F", 1, 2), ("F", 1, 1), ("I", 1, 1),
    ("B", 1, 3), ("R", 0, 4), ("G", 1, 4), ("K", 1, 4), ("A", 1, 4), ("J", 1, 2), ("D", 1, 0), ("H", 1, 3),
    ("B", 1, 4), ("D", 1, 2), ("J", 1, 1), ("D", 1, 1), ("Z", 1, 0), ("I", 1, 3), ("G", 1, 5), ("H", 1, 4),
    ("F", 1, 3), ("Z", 1, 2), ("K", 1, 5), ("I", 1, 4), ("A", 1, 5), ("Z", 1, 1), ("J", 1, 3), ("E", 1, 0),
    ("F", 1, 4), ("B", 1, 5), ("D", 1, 3), ("E", 1, 2), ("J", 1, 4), ("E", 1, 1), ("H", 1, 5), ("D", 1, 4),
    ("I", 1, 5), ("Z", 1, 3), ("F", 1, 5), ("W", 1, 1), ("Z", 1, 4), ("W", 1, 2), ("J", 1, 5), ("D", 1, 5),
    ("E", 1, 3), ("W", 1, 0), ("N", 1, 1), ("Z", 1, 5), ("E", 1, 4), ("W", 1, 3), ("E", 1, 5), ("N", 1, 2),
    ("W", 1, 4), ("W", 1, 5), ("N", 1, 4), ("N", 1, 3), ("N", 1, 0), ("N", 1, 5),
)

def kernel(
    sizes,
    tok,
    gw_hbm,
    uw_hbm,
    dw_hbm,
    gs,
    us,
    ds_,
    gain,
    taps,
    bias,
    out,
    gw,
    uw,
    dw,
    dwb,
    operand,
    rsb,
    stat,
    part,
    crecv,
    xsend,
    xrecv,
    hid,
    ysend,
    own,
    yrecv,
    zsend,
    zrecv,
    hnew,
    raw,
    wsem,
    lsem,
    ssem,
    sent,
    csem,
    xsem,
    hsem,
    osem,
    ysem,
    zsem,
    asem,
    fsem,
):
    chunks, n_tok, d_loc, f_loc, d_all, n_z = sizes
    layers = len(chunks)
    tiles = f_loc // LANES
    units = (tiles + 1) // 2
    pairs, middle = tiles // 2, units // 2
    piece, d_half = d_loc // (2 * n_z), d_loc // 2
    first = [sum(len(c) for c in chunks[:l]) for l in range(layers)]
    f32, bf16 = jnp.float32, jnp.bfloat16
    ra, cb = lax.axis_index("ra"), lax.axis_index("cb")
    z, y = ra // 2, ra % 2
    x, c = cb // 2, cb % 2
    core_dev = (ra, x * 2 + (1 - c))
    x_dev = (ra, (1 - x) * 2 + c)
    y_dev = (z * 2 + (1 - y), cb)

    def z_dev(i):
        return (lax.rem(z + i, n_z) * 2 + y, cb)

    def remote(src, dst, sems, dev):
        return pltpu.make_async_remote_copy(
            src_ref=src, dst_ref=dst, send_sem=sems[0], recv_sem=sems[1], device_id=dev, device_id_type=MESH
        )

    def span_of(at, width, size=1):
        return pl.ds(pl.multiple_of(at * width, width), size * width)

    def each(fn, begin=0, end=units):
        stop = min(end, pairs)
        if stop > begin:

            def step(u, carry):
                fn(u, 2)
                return carry

            lax.fori_loop(begin, stop, step, 0)
        if end > pairs:
            fn(pairs, 1)

    def first_load(u, w, n):
        src, dst = ((gw_hbm, gw), (uw_hbm, uw))[n]
        cols = span_of(u * 2, LANES, w)
        return pltpu.make_async_copy(src.at[0, :, cols], dst.at[0, :, cols], wsem.at[u, n])

    def load(l, n):
        src, dst = ((gw_hbm, gw), (uw_hbm, uw), (dw_hbm, dw))[n]
        return pltpu.make_async_copy(src.at[l], dst if n == 2 else dst.at[l], lsem.at[l, n])

    def start_first(u, w):
        first_load(u, w, 0).start()
        first_load(u, w, 1).start()

    each(start_first)

    def stat_copy(n, k):
        return remote(stat.at[n, 0], stat.at[n, k], (ssem.at[0, n], ssem.at[1, n]), (ra, lax.rem(cb + k, 4)))

    def picked(s, e):
        lane = lax.broadcasted_iota(jnp.int32, (e - s, LANES), 1)
        row = lax.broadcasted_iota(jnp.int32, (e - s, LANES), 0)
        return lane == lax.shift_right_logical(row + s, 3)

    def squares(n, h, l, s, e):
        wide = h[s:e, :].astype(f32)
        ssq = jnp.sum(wide * wide, axis=1, keepdims=True)
        packed = jnp.where(picked(s, e), jnp.broadcast_to(ssq, (e - s, LANES)), 0.0)
        stat[n, 0] = jnp.sum(packed.reshape((e - s) // 8, 8, LANES), axis=0)
        operand[s:e, :] = (wide * gain[l : l + 1, :]).astype(bf16)

    def share_squares(n):
        for k in range(1, 4):
            stat_copy(n, k).start()

    def scale_rows(n, s, e):
        others = stat.at[n, 1:4]
        remote(others, others, (ssem.at[0, n], ssem.at[1, n]), core_dev).wait()
        total = stat[n, 0] + stat[n, 1] + stat[n, 2] + stat[n, 3]
        spread = jnp.broadcast_to(total[None], ((e - s) // 8, 8, LANES)).reshape(e - s, LANES)
        summed = jnp.sum(jnp.where(picked(s, e), spread, 0.0), axis=1, keepdims=True)
        rsb[s:e, :] = jnp.broadcast_to(lax.rsqrt(summed / d_all + norm_eps), (e - s, LANES))

    def cast_down(l):
        load(l, 2).wait()

        def step(i, carry):
            r = span_of(i, LANES)
            dwb[l, r, :] = dw[r, :].astype(bf16)
            return carry

        lax.fori_loop(0, tiles, step, 0)
        if l + 1 < layers:
            load(l + 1, 2).start()

    def wait_sent(l, n):
        block = (
            part.at[0 : n_tok // 2, :],
            xsend,
            hid.at[l, 0 : 3 * n_tok // 4, :],
            ysend,
            zsend.at[:, 0 : (n_z - 1) * piece],
            hnew.at[l, :, 0 : (n_z - 1) * piece],
            hnew.at[l, :, 0:d_half],
        )[n]
        remote(block, block, (sent.at[l, n], csem.at[0, 0]), core_dev).wait_send()

    def steps_of(l, k):
        s, e = chunks[l][k]
        at = first[l] + k
        half, quarter = (e - s) // 2, (e - s) // 4
        lo, hi = max(s - PACK, 0), min(e + PACK, n_tok)
        h = tok if l == 0 else hnew.at[l - 1]

        def block_rows(cc, xx):
            return pl.ds(pl.multiple_of(s + cc * half + xx * quarter, PACK), quarter)

        def local_rows(xx):
            return pl.ds(pl.multiple_of(s // 2 + xx * quarter, PACK), quarter)

        x_rows = slice(s // 4, e // 4)

        def wide_cols(hf, width):
            return slice(0, middle * width) if hf == 0 else slice(middle * width, 2 * f_loc * width // (4 * LANES))

        def core_copy(hf):
            rows = pl.ds(pl.multiple_of(s + (1 - c) * half, PACK), half)
            cols = wide_cols(hf, 4 * LANES)
            return remote(part.at[rows, cols], crecv.at[l, s // 2 : e // 2, cols], (sent.at[l, 0], csem.at[at, hf]), core_dev)

        def x_copy(hf):
            cols = wide_cols(hf, 4 * LANES)
            return remote(xsend.at[x_rows, cols], xrecv.at[l, x_rows, cols], (sent.at[l, 1], xsem.at[at, hf]), x_dev)

        def h_copy(hf, n):
            block = hid.at[l, block_rows(c, 1 - x if n == 2 else x), wide_cols(hf, 2 * LANES)]
            return remote(block, block, (sent.at[l, 2], hsem.at[at, hf] if n == 0 else osem.at[at]), x_dev if n == 0 else core_dev)

        def y_copy(i):
            cols = span_of(lax.rem(z + i, n_z), piece)
            return remote(ysend.at[s:e, cols], yrecv.at[l, s:e, cols], (sent.at[l, 3], ysem.at[at, i - 1]), y_dev)

        def z_copy(i):
            cols = span_of(lax.rem(z + i, n_z), piece)
            return remote(zsend.at[s:e, cols], zrecv.at[l, i - 1, s:e, :], (sent.at[l, 4], zsem.at[at]), z_dev(i))

        def gather_z(i):
            block = hnew.at[l, s:e, span_of(y * n_z + z, piece)]
            return remote(block, block, (sent.at[l, 5], asem.at[at, i - 1]), z_dev(i))

        def gather_y(i):
            block = hnew.at[l, s:e, span_of(y * n_z + lax.rem(z + n_z - i, n_z), piece)]
            return remote(block, block, (sent.at[l, 6], fsem.at[at]), y_dev)

        def product(u, w):
            cols = span_of(u * 2, LANES, w)
            weights = jnp.concatenate([gw[l, :, cols].astype(bf16), uw[l, :, cols].astype(bf16)], axis=1)
            return jnp.dot(operand[lo:hi, :], weights, preferred_element_type=f32)

        def raw_unit(u, w):
            if l == 0:
                first_load(u, w, 0).wait()
                first_load(u, w, 1).wait()
            raw[0 : hi - lo, span_of(u * 4, LANES, 2 * w)] = product(u, w)

        def gate_unit(u, w):
            acc = raw[0 : hi - lo, span_of(u * 4, LANES, 2 * w)] if k == 0 else product(u, w)
            rs = rsb[lo:hi, :]
            rows = lax.broadcasted_iota(jnp.int32, rs.shape, 0)
            for i in range(w):
                col = span_of(u * 2 + i, LANES)
                g = acc[:, i * LANES : (i + 1) * LANES] * rs * gs[l : l + 1, col]
                prev, nxt = pltpu.roll(g, 1, 0), pltpu.roll(g, hi - lo - 1, 0)
                if s == 0:
                    prev = jnp.where(rows == 0, 0.0, prev)
                if e == n_tok:
                    nxt = jnp.where(rows == hi - lo - 1, 0.0, nxt)
                mixed = taps[0, l : l + 1, col] * prev + taps[1, l : l + 1, col] * g + taps[2, l : l + 1, col] * nxt
                upward = acc[:, (w + i) * LANES : (w + i + 1) * LANES] * rs * us[l : l + 1, col]
                part[s:e, span_of(u * 4 + 2 * i, LANES)] = mixed[s - lo : e - lo].astype(bf16)
                part[s:e, span_of(u * 4 + 2 * i + 1, LANES)] = upward[s - lo : e - lo].astype(bf16)

        def x_unit(u, w):
            cols = span_of(u * 4, LANES, 2 * w)
            mine = part[block_rows(c, 1 - x), cols].astype(f32)
            xsend[x_rows, cols] = (mine + crecv[l, local_rows(1 - x), cols].astype(f32)).astype(bf16)

        def hidden_unit(u, w):
            cols = span_of(u * 4, LANES, 2 * w)
            rows = block_rows(c, x)
            total = (
                part[rows, cols].astype(f32)
                + crecv[l, local_rows(x), cols].astype(f32)
                + xrecv[l, x_rows, cols].astype(f32)
            )
            for i in range(w):
                col = span_of(u * 2 + i, LANES)
                mixed = total[:, 2 * i * LANES : (2 * i + 1) * LANES] + bias[l : l + 1, col]
                upward = total[:, (2 * i + 1) * LANES : (2 * i + 2) * LANES]
                hid[l, rows, col] = (mixed / (1.0 + jnp.exp(-mixed)) * upward).astype(bf16)

        def bounds(hf):
            return (0, middle) if hf == 0 else (middle, units)

        def gate(hf):
            each(gate_unit, *bounds(hf))
            core_copy(hf).start()

        def reduce_x(hf):
            core_copy(hf).wait_recv()
            each(x_unit, *bounds(hf))
            x_copy(hf).start()

        def hidden(hf):
            x_copy(hf).wait_recv()
            each(hidden_unit, *bounds(hf))
            h_copy(hf, 0).start()
            h_copy(hf, 1).start()

        def forward_hidden(hf):
            h_copy(hf, 0).wait_recv()
            h_copy(hf, 2).start()

        def down():
            theirs = hid.at[l, pl.ds(pl.multiple_of(s + (1 - c) * half, PACK), half), :]
            remote(theirs, theirs, (sent.at[l, 2], osem.at[at]), core_dev).wait_recv()
            rows = hid[l, s:e, :]
            other = jnp.dot(rows, dwb[l, :, span_of(1 - y, d_half)], preferred_element_type=f32)
            ysend[s:e, :] = other.astype(bf16)
            for i in range(1, n_z + 1):
                y_copy(i).start()
            own[s:e, :] = jnp.dot(rows, dwb[l, :, span_of(y, d_half)], preferred_element_type=f32)

        def spread():
            for i in range(1, n_z):
                cols = span_of(lax.rem(z + i, n_z), piece)
                y_copy(i).wait_recv()
                zsend[s:e, cols] = (own[s:e, cols] + yrecv[l, s:e, cols].astype(f32)).astype(bf16)
                z_copy(i).start()

        def finish():
            cols, mine = span_of(z, piece), span_of(y * n_z + z, piece)
            y_copy(n_z).wait_recv()
            acc = own[s:e, cols] + yrecv[l, s:e, cols].astype(f32)
            pieces = zrecv.at[l, :, s:e, :]
            remote(pieces, pieces, (sent.at[l, 4], zsem.at[at]), y_dev).wait_recv()
            for i in range(1, n_z):
                acc = acc + zrecv[l, i - 1, s:e, :].astype(f32)
            new = residual_scale * h[s:e, mine].astype(f32) + acc * ds_[l : l + 1, mine]
            hnew[l, s:e, mine] = new.astype(bf16)
            for i in range(1, n_z):
                gather_z(i).start()
            gather_y(0).start()

        def forward():
            for i in range(1, n_z):
                gather_z(i).wait_recv()
                gather_y(i).start()

        def arrived():
            theirs = hnew.at[l, s:e, span_of(1 - y, d_half)]
            remote(theirs, theirs, (sent.at[l, 6], fsem.at[at]), y_dev).wait_recv()
            if l + 1 < layers:
                squares(1 + at, hnew.at[l], l + 1, s, e)
                share_squares(1 + at)
            else:
                out[s:e, :] = hnew[l, s:e, :]

        return {
            "M": functools.partial(each, raw_unit),
            "G": functools.partial(gate, 0),
            "K": functools.partial(gate, 1),
            "A": functools.partial(reduce_x, 0),
            "B": functools.partial(reduce_x, 1),
            "H": functools.partial(hidden, 0),
            "I": functools.partial(hidden, 1),
            "F": functools.partial(forward_hidden, 0),
            "J": functools.partial(forward_hidden, 1),
            "D": down,
            "Z": spread,
            "E": finish,
            "W": forward,
            "N": arrived,
            "R": functools.partial(scale_rows, 1 + at, s, e),
            "C": functools.partial(cast_down, l),
        }

    barrier = pltpu.get_barrier_semaphore()
    peers = [(ra, lax.rem(cb + k, 4)) for k in range(1, 4)] + [y_dev] + [z_dev(k) for k in range(1, n_z)]
    for dev in peers:
        pl.semaphore_signal(barrier, inc=1, device_id=dev, device_id_type=MESH)
    squares(0, tok, 0, 0, n_tok)
    pl.semaphore_wait(barrier, len(peers))

    share_squares(0)
    steps = {(l, k): steps_of(l, k) for l in range(layers) for k in range(len(chunks[l]))}
    begun = set()
    reused = {"G": 0, "A": 1, "D": 3, "Z": 4}
    for s, l, k in ORDER:
        if l > 0 and (s, l) not in begun and s in reused:
            wait_sent(l - 1, reused[s])
        begun.add((s, l))
        if s == "M" and l > 0:
            load(l, 0).wait()
            load(l, 1).wait()
        steps[l, k][s]()
        if (s, l) == ("M", 0):
            load(0, 2).start()
            for ll in range(1, layers):
                load(ll, 0).start()
                load(ll, 1).start()
            scale_rows(0, 0, n_tok)
    for l in range(layers):
        for n in range(7):
            if l == layers - 1 or n not in reused.values():
                wait_sent(l, n)


def fused(n_ra, tokens, gate_weight, up_weight, down_weight, gate_scale, up_scale, down_scale, gain, taps, bias, d_all):
    n_tok, d_loc = tokens.shape
    layers, _, f_loc = gate_weight.shape
    n_z = n_ra // 2
    chunks = row_chunks(n_tok)
    total = sum(len(c) for c in chunks)
    tiles = f_loc // LANES
    units = (tiles + 1) // 2
    f32, bf16 = jnp.float32, jnp.bfloat16
    dma = pltpu.SemaphoreType.DMA
    vmem, hbm = pl.BlockSpec(memory_space=pltpu.VMEM), pl.BlockSpec(memory_space=pl.ANY)
    return pl.pallas_call(
        functools.partial(kernel, (chunks, n_tok, d_loc, f_loc, d_all, n_z)),
        out_shape=pltpu.VMEM((n_tok, d_loc), bf16),
        in_specs=[vmem, hbm, hbm, hbm] + [vmem] * 6,
        out_specs=vmem,
        scratch_shapes=[
            pltpu.VMEM((layers, d_loc, f_loc), f32),
            pltpu.VMEM((layers, d_loc, f_loc), f32),
            pltpu.VMEM((f_loc, d_loc), f32),
            pltpu.VMEM((layers, f_loc, d_loc), bf16),
            pltpu.VMEM((n_tok, d_loc), bf16),
            pltpu.VMEM((n_tok, LANES), f32),
            pltpu.VMEM((1 + total, 4, 8, LANES), f32),
            pltpu.VMEM((n_tok, 2 * f_loc), bf16),
            pltpu.VMEM((layers, n_tok // 2, 2 * f_loc), bf16),
            pltpu.VMEM((n_tok // 4, 2 * f_loc), bf16),
            pltpu.VMEM((layers, n_tok // 4, 2 * f_loc), bf16),
            pltpu.VMEM((layers, n_tok, f_loc), bf16),
            pltpu.VMEM((n_tok, d_loc // 2), bf16),
            pltpu.VMEM((n_tok, d_loc // 2), f32),
            pltpu.VMEM((layers, n_tok, d_loc // 2), bf16),
            pltpu.VMEM((n_tok, d_loc // 2), bf16),
            pltpu.VMEM((layers, n_z - 1, n_tok, d_loc // n_ra), bf16),
            pltpu.VMEM((layers, n_tok, d_loc), bf16),
            pltpu.VMEM((chunks[0][0][1] + PACK, 2 * f_loc), f32),
            dma((units, 2)),
            dma((layers, 3)),
            dma((2, 1 + total)),
            dma((layers, 7)),
            dma((total, 2)),
            dma((total, 2)),
            dma((total, 2)),
            dma((total,)),
            dma((total, n_z)),
            dma((total,)),
            dma((total, n_z - 1)),
            dma((total,)),
        ],
        compiler_params=pltpu.CompilerParams(
            collective_id=0, has_side_effects=True, vmem_limit_bytes=60_000_000
        ),
    )(tokens, gate_weight, up_weight, down_weight, gate_scale, up_scale, down_scale, gain, jnp.transpose(taps, (1, 0, 2)), bias)


def plain(tokens, gate_weight, up_weight, down_weight, gate_scale, up_scale, down_scale, gain, conv_taps, bias, d_all):
    hstate = tokens
    for layer in range(gate_weight.shape[0]):
        wide = hstate.astype(jnp.float32)
        squares = jnp.sum(wide * wide, axis=1)
        operand = (wide * gain[layer]).astype(jnp.bfloat16)
        gate_part = jnp.dot(operand, gate_weight[layer].astype(jnp.bfloat16), preferred_element_type=jnp.float32)
        up_part = jnp.dot(operand, up_weight[layer].astype(jnp.bfloat16), preferred_element_type=jnp.float32)
        gate_sum, up_sum, square_sum = lax.psum((gate_part, up_part, squares), "cb")
        rscale = lax.rsqrt(square_sum / d_all + norm_eps)[:, None]
        gate = gate_sum * rscale * gate_scale[layer]
        upward = up_sum * rscale * up_scale[layer]
        padded = jnp.pad(gate, ((1, 1), (0, 0)))
        taps = conv_taps[layer]
        mixed = taps[0] * padded[:-2] + taps[1] * padded[1:-1] + taps[2] * padded[2:] + bias[layer]
        hidden = (jax.nn.silu(mixed) * upward).astype(jnp.bfloat16)
        term = jnp.dot(hidden, down_weight[layer].astype(jnp.bfloat16), preferred_element_type=jnp.float32)
        branch = lax.psum(term, "ra") * down_scale[layer]
        hstate = (residual_scale * wide + branch).astype(jnp.bfloat16)
    return hstate


def solution(mesh):
    n_ra, n_cb = mesh.shape["ra"], mesh.shape["cb"]

    def per_device(*args):
        n_tok, d_loc = args[0].shape
        f_loc = args[1].shape[2]
        fits = n_cb == 4 and n_ra % 2 == 0 and n_ra >= 4 and n_tok % (8 * 4 * PACK) == 0 and n_tok <= 8 * LANES
        fits = fits and f_loc % LANES == 0 and d_loc % (LANES * n_ra) == 0 and f_loc >= 4 * LANES and args[1].shape[0] == len(ENDS)
        if fits:
            return fused(n_ra, *args, d_loc * n_cb)
        return plain(*args, d_loc * n_cb)

    in_specs = (
        P(None, "cb"),
        P(None, "cb", "ra"),
        P(None, "cb", "ra"),
        P(None, "ra", "cb"),
        P(None, "ra"),
        P(None, "ra"),
        P(None, "cb"),
        P(None, "cb"),
        P(None, None, "ra"),
        P(None, "ra"),
    )
    return jax.shard_map(
        per_device, mesh=mesh, in_specs=in_specs, out_specs=P(None, "cb"), check_vma=False
    )
```
